32 devices in a mesh: sp: 8 (over z, y), tp: 4 (over x, core).
Axes of the slice: x: 2, y: 2, z: 4, core: 2. Of those that a mesh axis runs over, the one named last changes fastest.
Arguments:
- inputs: bfloat16 [4096, 4096], P('sp', 'tp'), may hold values from -24 to 24
- length: int32 [1], replicated, may hold values from 2049 to 4096
- win_query: bfloat16 [4096, 1536], P(None, 'tp'), may hold values from -8 to 8
- win_key: bfloat16 [4096, 512], P(None, 'tp'), may hold values from -8 to 8
- win_value: bfloat16 [4096, 512], P(None, 'tp'), may hold values from -1.5 to 1.5
- sink_logit: float32 [24], P('tp'), may hold values from 4 to 8
- diff_query: bfloat16 [4096, 1024], P(None, 'tp'), may hold values from -8 to 8
- diff_key: bfloat16 [4096, 1024], P(None, 'tp'), may hold values from -8 to 8
- diff_value: bfloat16 [4096, 1024], P(None, 'tp'), may hold values from -0.09375 to 0.09375
- mix_lambda: float32 [16], P('tp'), may hold values from 0.3 to 0.8
- head_gain: float32 [64], replicated, may hold values from 0.1 to 1.9
- win_out: bfloat16 [1536, 4096], P('tp'), may hold values from -0.125 to 0.125
- diff_out: bfloat16 [1024, 4096], P('tp'), may hold values from -0.125 to 0.125
Outputs:
- merged_out: bfloat16 [4096, 4096], P(('sp', 'tp'))
The draws below stay inside these ranges and needn't reach their ends.
All inputs are finite; a program needn't handle non-finite values.
Results may differ from the reference program's by a relative error of at most 0.015.
Values may be sent and summed in bfloat16 or wider, within the bound.
A program may use at most 128 MiB of HBM per device.

```python
import jax
import jax.numpy as jnp
from jax import lax

D = 4096
HEAD = 64
DQK = 32
WKV = 8
GROUP = 3
WQH = 24
DH = 16
WINDOW = 128
TOKENS = 4096
N_TP = 4


def clipped(key, shape):
    return jnp.clip(jax.random.normal(key, shape, jnp.float32), -6.0, 6.0)


def window_pair(key):
    key_weight = clipped(jax.random.fold_in(key, 101), (D, WKV * HEAD)) * D ** (-0.5)
    noise_part = clipped(jax.random.fold_in(key, 102), (D, WKV * GROUP * HEAD)) * D ** (-0.5)
    query_weight = noise_part
    return (query_weight, key_weight)


def diff_pair(key):
    key_weight = clipped(jax.random.fold_in(key, 201), (D, DH * 2 * DQK)) * D ** (-0.5)
    noise_part = clipped(jax.random.fold_in(key, 202), (D, DH * 2 * DQK)) * (3.0 / D) ** 0.5
    query_weight = noise_part
    return (query_weight, key_weight)


def draw_inputs(key, part):
    base_rows = clipped(jax.random.fold_in(key, 301), (TOKENS, D))
    return base_rows.astype(jnp.bfloat16)


def draw_win_query(key, part):
    return window_pair(key)[0].astype(jnp.bfloat16)


def draw_win_key(key, part):
    return window_pair(key)[1].astype(jnp.bfloat16)


def draw_diff_query(key, part):
    return diff_pair(key)[0].astype(jnp.bfloat16)


def draw_diff_key(key, part):
    return diff_pair(key)[1].astype(jnp.bfloat16)


def block_scale(key, dims, cuts, low, top_value):
    gain, own = 1.0, jax.random.fold_in(key, 6)
    for dim, shards_of in cuts:
        steps = jnp.exp(jax.random.uniform(jax.random.fold_in(own, dim), (shards_of,), jnp.float32, low / len(cuts), top_value / len(cuts)))
        gain = gain * jnp.repeat(steps, dims[dim] // shards_of).reshape([-1 if axis == dim else 1 for axis in range(len(dims))])
    return gain


def gaussian(stream_key, shape, deviation, most, pieces=(), dtype=jnp.bfloat16):
    array = jax.random.normal(stream_key, shape, jnp.float32) * deviation
    if len(pieces) > 0:
        array = block_scale(stream_key, shape, pieces, -0.22, 0.18) * array
    return jnp.clip(array, min=-most, max=most).astype(dtype)


def setup_inputs(seed: int = 0) -> dict:
    splits = jax.random.split(jax.random.key(seed), 14)
    return {
        "inputs": draw_inputs(jax.random.fold_in(splits[13], 71), 0),
        "length": jax.random.randint(splits[1], (1,), TOKENS // 2 + 1, TOKENS + 1).astype(jnp.int32),
        "win_query": draw_win_query(jax.random.fold_in(splits[13], 71), 0),
        "win_key": draw_win_key(jax.random.fold_in(splits[13], 71), 0),
        "win_value": gaussian(splits[4], (D, WKV * HEAD), (max(D // 256, 1)) ** -0.5, 1.5, ((1, 4),)),
        "sink_logit": jnp.clip(4.0 + 4.0 * jax.random.uniform(splits[5], (WQH,), jnp.float32) ** block_scale(splits[5], (WQH,), ((0, 4),), -0.2, 0.2), 4.0, 8.0),
        "diff_query": draw_diff_query(jax.random.fold_in(splits[13], 71), 0),
        "diff_key": draw_diff_key(jax.random.fold_in(splits[13], 71), 0),
        "diff_value": gaussian(splits[8], (D, DH * HEAD), D ** -0.5, 0.09375, ((1, 4),)),
        "mix_lambda": jnp.clip(0.3 + 0.5 * jax.random.uniform(splits[9], (DH,), jnp.float32) ** block_scale(splits[9], (DH,), ((0, 4),), -0.2, 0.2), 0.3, 0.8),
        "head_gain": jnp.clip(1.0 + 0.18 * jax.random.normal(splits[10], (HEAD,), jnp.float32), 0.1, 1.9),
        "win_out": gaussian(splits[11], (WQH * HEAD, D), ((WQH + DH) * HEAD) ** -0.5, 0.125, ((0, 4),)),
        "diff_out": gaussian(splits[12], (DH * HEAD, D), ((WQH + DH) * HEAD) ** -0.5, 0.125, ((0, 4),)),
    }


epsilon = 1e-06
masked_score = -1e+30

def window_attention(win_q, win_k, win_v, sink_logit, live_count):
    queries = win_q.reshape(TOKENS, WKV, GROUP, HEAD)
    padded_k = jnp.pad(win_k.reshape(TOKENS, WKV, HEAD), ((WINDOW, WINDOW), (0, 0), (0, 0)))
    padded_v = jnp.pad(win_v.reshape(TOKENS, WKV, HEAD), ((WINDOW, WINDOW), (0, 0), (0, 0)))
    sink_table = sink_logit.reshape(WKV, GROUP)
    block_rows = 512
    block_count = TOKENS // block_rows

    def one_block(block_index):
        first_row = (block_index * block_rows).astype(jnp.int32)
        query_slab = lax.dynamic_slice_in_dim(queries, first_row, block_rows, 0).astype(jnp.float32)
        key_slab = lax.dynamic_slice_in_dim(padded_k, first_row, block_rows + 2 * WINDOW, 0).astype(jnp.float32)
        value_slab = lax.dynamic_slice_in_dim(padded_v, first_row, block_rows + 2 * WINDOW, 0).astype(jnp.float32)
        query_pos = first_row + jnp.arange(block_rows).astype(jnp.int32)
        key_pos = first_row - WINDOW + jnp.arange(block_rows + 2 * WINDOW).astype(jnp.int32)
        allowed = (jnp.abs(query_pos[:, None] - key_pos[None, :]) <= WINDOW) & (key_pos[None, :] >= 0) & (key_pos[None, :] < live_count)
        scores = jnp.einsum('qhgd,khd->hgqk', query_slab, key_slab) * HEAD ** (-0.5)
        scores = jnp.where(allowed[None, None], scores, masked_score)
        row_max = jnp.maximum(lax.optimization_barrier(jnp.max(scores, axis=-1)), sink_table[:, :, None])
        exponent = jnp.where(allowed[None, None], jnp.exp(scores - row_max[..., None]), 0.0)
        denominator = lax.optimization_barrier(jnp.sum(exponent, axis=-1)) + jnp.exp(sink_table[:, :, None] - row_max)
        weights_low = lax.optimization_barrier(exponent.astype(jnp.bfloat16)).astype(jnp.float32)
        result = jnp.einsum('hgqk,khd->qhgd', weights_low, value_slab) / jnp.transpose(denominator, (2, 0, 1))[..., None]
        result = jnp.where((query_pos < live_count)[:, None, None, None], result, 0.0)
        return result.reshape(block_rows, WQH * HEAD).astype(jnp.bfloat16)
    return lax.map(one_block, jnp.arange(block_count)).reshape(TOKENS, WQH * HEAD)

def diff_attention(diff_q, diff_k, diff_v, mix_lambda, head_gain, live_count):
    queries = diff_q.reshape(TOKENS, DH, 2, DQK)
    key_all = diff_k.reshape(TOKENS, DH, 2, DQK)
    value_all = diff_v.reshape(TOKENS, DH, HEAD)
    key_live = jnp.arange(TOKENS).astype(jnp.int32) < live_count
    block_rows = 512
    block_count = TOKENS // block_rows

    def one_head(head_index):
        query_head = lax.dynamic_index_in_dim(queries, head_index, 1, keepdims=False).astype(jnp.float32)
        key_head = lax.dynamic_index_in_dim(key_all, head_index, 1, keepdims=False).astype(jnp.float32)
        value_head = lax.dynamic_index_in_dim(value_all, head_index, 1, keepdims=False).astype(jnp.float32)
        mix_weight = lax.dynamic_index_in_dim(mix_lambda, head_index, 0, keepdims=False)

        def one_block(block_index):
            first_row = (block_index * block_rows).astype(jnp.int32)
            query_slab = lax.dynamic_slice_in_dim(query_head, first_row, block_rows, 0)
            scores = jnp.einsum('qmd,kmd->mqk', query_slab, key_head) * DQK ** (-0.5)
            scores = jnp.where(key_live[None, None], scores, masked_score)
            row_max = lax.optimization_barrier(jnp.max(scores, axis=-1, keepdims=True))
            exponent = jnp.where(key_live[None, None], jnp.exp(scores - row_max), 0.0)
            total_sum = lax.optimization_barrier(jnp.sum(exponent, axis=-1))
            weights_low = lax.optimization_barrier(exponent.astype(jnp.bfloat16)).astype(jnp.float32)
            map_rows = jnp.einsum('mqk,kd->mqd', weights_low, value_head) / total_sum[..., None]
            mixed_rows = map_rows[0] - mix_weight * map_rows[1]
            normed = mixed_rows * lax.rsqrt(lax.optimization_barrier(jnp.mean(mixed_rows * mixed_rows, axis=-1, keepdims=True)) + epsilon) * head_gain
            query_pos = first_row + jnp.arange(block_rows).astype(jnp.int32)
            return jnp.where((query_pos < live_count)[:, None], normed, 0.0)
        return lax.map(one_block, jnp.arange(block_count)).reshape(TOKENS, HEAD)
    result = lax.map(one_head, jnp.arange(DH))
    return jnp.transpose(result, (1, 0, 2)).reshape(TOKENS, DH * HEAD).astype(jnp.bfloat16)

def reference(inputs, length, win_query, win_key, win_value, sink_logit, diff_query, diff_key, diff_value, mix_lambda, head_gain, win_out, diff_out):
    live_count = length[0]

    def project(weight):
        return jnp.dot(inputs, weight, preferred_element_type=jnp.float32).astype(jnp.bfloat16)
    win_rows = window_attention(project(win_query), project(win_key), project(win_value), sink_logit, live_count)
    diff_rows = diff_attention(project(diff_query), project(diff_key), project(diff_value), mix_lambda, head_gain, live_count)
    win_cols = WQH // N_TP * HEAD
    diff_cols = DH // N_TP * HEAD
    merged = jnp.zeros((TOKENS, D), jnp.float32)
    for group_index in range(N_TP):
        partial_value = jnp.dot(win_rows[:, group_index * win_cols:(group_index + 1) * win_cols], win_out[group_index * win_cols:(group_index + 1) * win_cols], preferred_element_type=jnp.float32)
        partial_value = partial_value + jnp.dot(diff_rows[:, group_index * diff_cols:(group_index + 1) * diff_cols], diff_out[group_index * diff_cols:(group_index + 1) * diff_cols], preferred_element_type=jnp.float32)
        partial_value = lax.optimization_barrier(partial_value.astype(jnp.bfloat16)).astype(jnp.float32)
        merged = merged + partial_value
    return merged.astype(jnp.bfloat16)
```

```python
import functools

import jax
import jax.numpy as jnp
from jax import lax
from jax.experimental import pallas as pl
from jax.experimental.pallas import tpu as pltpu
from jax.sharding import PartitionSpec as P

HEAD = 64
DQK = 32
GROUP = 3
WINDOW = 128
LOG2E = 1.4426950408889634
NEG = -1e30
EPS = 1e-06
MESH = pl.DeviceIdType.MESH
VM = pl.BlockSpec(memory_space=pltpu.VMEM)
SM = pl.BlockSpec(memory_space=pltpu.SMEM)
F32 = jnp.float32
BF16 = jnp.bfloat16


def dot(a, b):
    return jnp.dot(a, b, preferred_element_type=F32)


def ring_to_sp(r, n):
    half = r // (n // 2)
    return (1 - half) * (2 * r) + half * (2 * (n - 1 - r) + 1)


def attention_kernel(
    n, length, sink, lam, gain, wqT, wk, wvT, dqT, dk, dvT,
    out, kbuf, vbuf, kwin, vwin, qz, acc, mx, ksem, vsem, hsem, lsem,
):
    rows = wk.shape[0]
    heads = dqT.shape[0] // HEAD
    kvh = wk.shape[1] // HEAD
    kw = min(2 * HEAD, wk.shape[1])
    sp = lax.axis_index("sp")
    y = sp % 2
    z = sp // 2
    me = z + y * (n - 1 - 2 * z)
    half = n // 2
    right = ring_to_sp((me + 1) % n, n)
    left = ring_to_sp((me + n - 1) % n, n)
    nxt = (sp + 1) % n
    prv = (sp + n - 1) % n
    barrier = pltpu.get_barrier_semaphore()
    for d in (left, right, prv, nxt):
        pl.semaphore_signal(barrier, inc=1, device_id={"sp": d}, device_id_type=MESH)
    pl.semaphore_wait(barrier, 4)

    W = WINDOW
    halos = []
    for i, (src, dst, to) in enumerate((
        (wk.at[pl.ds(rows - W, W)], kwin.at[pl.ds(0, W)], nxt),
        (wvT.at[:, pl.ds(rows - W, W)], vwin.at[:, pl.ds(0, W)], nxt),
        (wk.at[pl.ds(0, W)], kwin.at[pl.ds(rows + W, W)], prv),
        (wvT.at[:, pl.ds(0, W)], vwin.at[:, pl.ds(rows + W, W)], prv),
    )):
        c = pltpu.make_async_remote_copy(
            src_ref=src, dst_ref=dst, send_sem=hsem.at[0, i], recv_sem=hsem.at[1, i],
            device_id={"sp": to}, device_id_type=MESH)
        c.start()
        halos.append(c)

    def kcopy(direction, s, first=False):
        slot = (me + n - s) % n if direction == 0 else (me + s) % n
        return pltpu.make_async_remote_copy(
            src_ref=dk if first else kbuf.at[slot], dst_ref=kbuf.at[slot],
            send_sem=ksem.at[0, direction, s], recv_sem=ksem.at[1, direction, s],
            device_id={"sp": right if direction == 0 else left}, device_id_type=MESH)

    def vcopy(direction, s, first=False):
        slot = (me + n - s) % n if direction == 0 else (me + s) % n
        return pltpu.make_async_remote_copy(
            src_ref=dvT if first else vbuf.at[slot], dst_ref=vbuf.at[slot],
            send_sem=vsem.at[0, direction, s], recv_sem=vsem.at[1, direction, s],
            device_id={"sp": right if direction == 0 else left}, device_id_type=MESH)

    for d in (0, 1):
        kcopy(d, 0, True).start()
        vcopy(d, 0, True).start()

    local = [
        pltpu.make_async_copy(wk, kwin.at[pl.ds(W, rows)], lsem.at[0]),
        pltpu.make_async_copy(wvT, vwin.at[:, pl.ds(W, rows)], lsem.at[1]),
    ]
    live = length[0]
    offset = sp * rows
    rowid = lax.broadcasted_iota(jnp.int32, (128, rows), 0) // DQK
    for h in range(heads):
        tile = dqT[(h // 2) * 128:(h // 2) * 128 + 128, :]
        for m in (0, 1):
            keep = jnp.where(rowid == (h % 2) * 2 + m, 1.0, 0.0).astype(BF16)
            qz[h, m] = tile * keep
    mx[...] = jnp.full(mx.shape, NEG, F32)
    acc[...] = jnp.zeros(acc.shape, F32)

    def block(ksrc, vsrc, origin):
        spo = ring_to_sp(origin, n)
        start = spo * rows
        kpos = start + lax.broadcasted_iota(jnp.int32, (rows, 1), 0)
        klive = kpos < live
        vpos = start + lax.broadcasted_iota(jnp.int32, (1, rows), 1)
        vlive = jnp.where(vpos < live, 1.0, 0.0).astype(BF16)
        ones = jnp.broadcast_to(vlive, (16, rows))

        def head(h, carry):
            kt = ksrc[:, pl.ds(pl.multiple_of((h // 2) * 128, 128), 128)]
            vt = vsrc[pl.ds(pl.multiple_of(h * HEAD, HEAD), HEAD), :] * vlive
            vx = jnp.concatenate([vt, ones], axis=0)
            for m in (0, 1):
                for q0 in range(0, rows, 256):
                    cols = pl.ds(q0, 256)
                    s = dot(kt, qz[h, m, :, cols])
                    s = jnp.where(klive, s, NEG)
                    old = mx[h, m, :, cols]
                    new = jnp.maximum(old, jnp.max(s, axis=0, keepdims=True))
                    p = jnp.exp2(s - new).astype(BF16)
                    acc[h, m, :, cols] = acc[h, m, :, cols] * jnp.exp2(old - new) + dot(vx, p)
                    mx[h, m, :, cols] = new
            return carry

        lax.fori_loop(0, heads, head, 0)

    block(dk, dvT, me)
    for c in local[:2]:
        c.start()
    for c in local[:2]:
        c.wait()
    for c in halos:
        c.wait()

    krel = lax.broadcasted_iota(jnp.int32, (3 * W, W), 0)
    qrel = lax.broadcasted_iota(jnp.int32, (3 * W, W), 1)
    band = jnp.abs(krel - W - qrel) <= W
    krow = lax.broadcasted_iota(jnp.int32, (1, 3 * W), 1)
    zeros = jnp.zeros((HEAD, GROUP * W), BF16)

    def qblock(b, carry):
        base = offset + b * W - W
        kp = base + krel
        allowed = band & (kp >= 0) & (kp < live)
        bias = jnp.where(allowed, 0.0, NEG)
        bias = jnp.concatenate([bias] * GROUP, axis=1)
        vp = base + krow
        vlive = jnp.where((vp >= 0) & (vp < live), 1.0, 0.0).astype(BF16)
        ones = jnp.broadcast_to(vlive, (16, 3 * W))
        qlane = offset + b * W + lax.broadcasted_iota(jnp.int32, (1, W), 1)
        qlive = qlane < live
        at = pl.multiple_of(b * W, W)
        for j in range(kvh):
            lo = j * HEAD // kw * kw
            ks = kwin[pl.ds(at, 3 * W), lo:lo + kw]
            vt = vwin[j * HEAD:(j + 1) * HEAD, pl.ds(at, 3 * W)] * vlive
            vx = jnp.concatenate([vt, ones], axis=0)
            q = jnp.concatenate(
                [wqT[(j * GROUP + g) * HEAD:(j * GROUP + g + 1) * HEAD, pl.ds(at, W)] for g in range(GROUP)],
                axis=1)
            if kw > HEAD:
                q = jnp.concatenate([q, zeros] if j % 2 == 0 else [zeros, q], axis=0)
            s = dot(ks, q) + bias
            snk = jnp.concatenate(
                [jnp.full((1, W), sink[j * GROUP + g] * LOG2E, F32) for g in range(GROUP)], axis=1)
            top = jnp.maximum(snk, jnp.max(s, axis=0, keepdims=True))
            p = jnp.exp2(s - top).astype(BF16)
            o = dot(vx, p)
            r = o[:HEAD] / (o[HEAD:HEAD + 1] + jnp.exp2(snk - top))
            for g in range(GROUP):
                piece = jnp.where(qlive, r[:, g * W:(g + 1) * W], 0.0).astype(BF16)
                out[(j * GROUP + g) * HEAD:(j * GROUP + g + 1) * HEAD, pl.ds(at, W)] = piece
        return carry

    lax.fori_loop(0, rows // W, qblock, 0)

    def step(s, carry):
        kcopy(0, s).wait_recv()
        kcopy(0, s + 1).start()
        vcopy(1, s).wait_recv()
        vcopy(1, s + 1).start()
        vcopy(0, s).wait_recv()
        kcopy(1, s).wait_recv()

        @pl.when(s < half - 2)
        def _():
            vcopy(0, s + 1).start()
            kcopy(1, s + 1).start()

        def side(i, c):
            origin = (me + n + (2 * i - 1) * (s + 1)) % n
            block(kbuf.at[origin], vbuf.at[origin], origin)
            return c

        lax.fori_loop(0, 2, side, 0)
        return carry

    lax.fori_loop(0, half - 1, step, 0)
    kcopy(0, half - 1).wait_recv()
    vcopy(1, half - 1).wait_recv()
    far = (me + half) % n
    block(kbuf.at[far], vbuf.at[far], far)

    qlive = offset + lax.broadcasted_iota(jnp.int32, (1, rows), 1) < live
    base = wqT.shape[0]
    for h in range(heads):
        a0 = acc[h, 0]
        a1 = acc[h, 1]
        t0 = a0[HEAD:HEAD + 1]
        t1 = a1[HEAD:HEAD + 1]
        mixed = a0[:HEAD] / t0 - lam[h] * (a1[:HEAD] / t1)
        ms = jnp.mean(mixed * mixed, axis=0, keepdims=True)
        r = mixed * lax.rsqrt(ms + EPS) * gain[...]
        out[base + h * HEAD:base + (h + 1) * HEAD, :] = jnp.where(qlive, r, 0.0).astype(BF16)

    for d in (0, 1):
        for s in range(half):
            if s < half - 1 or d == 0:
                kcopy(d, s, s == 0).wait_send()
            if s < half - 1 or d == 1:
                vcopy(d, s, s == 0).wait_send()


def attention(n, length, sink, lam, gain, wqT, wk, wvT, dqT, dk, dvT):
    rows = wk.shape[0]
    heads = dqT.shape[0] // HEAD
    half = n // 2
    return pl.pallas_call(
        functools.partial(attention_kernel, n),
        out_shape=jax.ShapeDtypeStruct((wqT.shape[0] + dqT.shape[0], rows), BF16),
        in_specs=[SM, SM, SM] + [VM] * 7,
        out_specs=VM,
        scratch_shapes=[
            pltpu.VMEM((n,) + dk.shape, BF16),
            pltpu.VMEM((n,) + dvT.shape, BF16),
            pltpu.VMEM((rows + 2 * WINDOW, wk.shape[1]), BF16),
            pltpu.VMEM((wvT.shape[0], rows + 2 * WINDOW), BF16),
            pltpu.VMEM((heads, 2, 128, rows), BF16),
            pltpu.VMEM((heads, 2, HEAD + 16, rows), F32),
            pltpu.VMEM((heads, 2, 1, rows), F32),
            pltpu.SemaphoreType.DMA((2, 2, half)),
            pltpu.SemaphoreType.DMA((2, 2, half)),
            pltpu.SemaphoreType.DMA((2, 4)),
            pltpu.SemaphoreType.DMA((2,)),
        ],
        compiler_params=pltpu.CompilerParams(
            collective_id=1, has_side_effects=True, vmem_limit_bytes=60 * 1024 * 1024),
        name="attention",
    )(length, sink, lam, gain, wqT, wk, wvT, dqT, dk, dvT)


def body(n, inputs, length, win_query, win_key, win_value, sink_logit, diff_query, diff_key,
         diff_value, mix_lambda, head_gain, win_out, diff_out):
    seg = lax.all_gather(inputs, "tp", axis=1, tiled=True)
    wq = (dot(seg, win_query) * (HEAD ** -0.5 * LOG2E)).astype(BF16)
    wk = dot(seg, win_key).astype(BF16)
    wv = dot(seg, win_value).astype(BF16)
    dq = (dot(seg, diff_query) * (DQK ** -0.5 * LOG2E)).astype(BF16)
    dk = dot(seg, diff_key).astype(BF16)
    dv = dot(seg, diff_value).astype(BF16)
    rowsT = attention(n, length, sink_logit, mix_lambda, head_gain.reshape(-1, 1),
                      wq.T, wk, wv.T, dq.T, dk, dv.T)
    cut = win_out.shape[0]
    contract = (((0,), (0,)), ((), ()))
    part = lax.dot_general(rowsT[:cut], win_out, contract, preferred_element_type=F32)
    part += lax.dot_general(rowsT[cut:], diff_out, contract, preferred_element_type=F32)
    return lax.psum_scatter(part.astype(BF16), "tp", scatter_dimension=0, tiled=True)


def solution(mesh):
    placed = (
        P("sp", "tp"), P(), P(None, "tp"), P(None, "tp"), P(None, "tp"), P("tp"), P(None, "tp"),
        P(None, "tp"), P(None, "tp"), P("tp"), P(), P("tp", None), P("tp", None),
    )
    return jax.shard_map(
        functools.partial(body, mesh.shape["sp"]), mesh=mesh, in_specs=placed,
        out_specs=P(("sp", "tp"), None), check_vma=False)
```

```python
import functools

import jax
import jax.numpy as jnp
from jax import lax
from jax.experimental import pallas as pl
from jax.experimental.pallas import tpu as pltpu
from jax.sharding import PartitionSpec as P

HEAD = 64
DQK = 32
GROUP = 3
WINDOW = 128
LOG2E = 1.4426950408889634
NEG = -1e30
EPS = 1e-06
MESH = pl.DeviceIdType.MESH
VM = pl.BlockSpec(memory_space=pltpu.VMEM)
ANY = pl.BlockSpec(memory_space=pl.ANY)
SM = pl.BlockSpec(memory_space=pltpu.SMEM)
F32 = jnp.float32
BF16 = jnp.bfloat16


def dot(a, b):
    return jnp.dot(a, b, preferred_element_type=F32)


def ring_to_sp(r, n):
    half = r // (n // 2)
    return (1 - half) * (2 * r) + half * (2 * (n - 1 - r) + 1)


def attention_kernel(
    n, length, sink, lam, gain, wqT, wk, wvT, dqT, dk, dvT, wo, do,
    out_rows, wpeer, out, kbuf, vbuf, kwin, vwin, qz, acc, mx, ksem, vsem, hsem, lsem, wsem,
):
    rows = wk.shape[0]
    heads = dqT.shape[0] // HEAD
    kvh = wk.shape[1] // HEAD
    kw = min(2 * HEAD, wk.shape[1])
    sp = lax.axis_index("sp")
    y = sp % 2
    z = sp // 2
    me = z + y * (n - 1 - 2 * z)
    half = n // 2
    right = ring_to_sp((me + 1) % n, n)
    left = ring_to_sp((me + n - 1) % n, n)
    nxt = (sp + 1) % n
    prv = (sp + n - 1) % n
    barrier = pltpu.get_barrier_semaphore()
    for d in (left, right, prv, nxt):
        pl.semaphore_signal(barrier, inc=1, device_id={"sp": d}, device_id_type=MESH)
    tp = lax.axis_index("tp")
    peer = tp + 1 - 2 * (tp % 2)
    pl.semaphore_signal(barrier, inc=1, device_id={"tp": peer}, device_id_type=MESH)
    pl.semaphore_wait(barrier, 5)

    W = WINDOW
    halos = []
    for i, (src, dst, to) in enumerate((
        (wk.at[pl.ds(rows - W, W)], kwin.at[pl.ds(0, W)], nxt),
        (wvT.at[:, pl.ds(rows - W, W)], vwin.at[:, pl.ds(0, W)], nxt),
        (wk.at[pl.ds(0, W)], kwin.at[pl.ds(rows + W, W)], prv),
        (wvT.at[:, pl.ds(0, W)], vwin.at[:, pl.ds(rows + W, W)], prv),
    )):
        c = pltpu.make_async_remote_copy(
            src_ref=src, dst_ref=dst, send_sem=hsem.at[0, i], recv_sem=hsem.at[1, i],
            device_id={"sp": to}, device_id_type=MESH)
        c.start()
        halos.append(c)

    def kcopy(direction, s, first=False):
        slot = (me + n - s) % n if direction == 0 else (me + s) % n
        return pltpu.make_async_remote_copy(
            src_ref=dk if first else kbuf.at[slot], dst_ref=kbuf.at[slot],
            send_sem=ksem.at[0, direction, s], recv_sem=ksem.at[1, direction, s],
            device_id={"sp": right if direction == 0 else left}, device_id_type=MESH)

    def vcopy(direction, s, first=False):
        slot = (me + n - s) % n if direction == 0 else (me + s) % n
        return pltpu.make_async_remote_copy(
            src_ref=dvT if first else vbuf.at[slot], dst_ref=vbuf.at[slot],
            send_sem=vsem.at[0, direction, s], recv_sem=vsem.at[1, direction, s],
            device_id={"sp": right if direction == 0 else left}, device_id_type=MESH)

    for d in (0, 1):
        kcopy(d, 0, True).start()
        vcopy(d, 0, True).start()

    cut = wo.shape[0]
    shared = [
        pltpu.make_async_remote_copy(
            src_ref=src, dst_ref=wpeer.at[pl.ds(at, src.shape[0])], send_sem=wsem.at[0, i],
            recv_sem=wsem.at[1, i], device_id={"tp": peer}, device_id_type=MESH)
        for i, (src, at) in enumerate(((wo, 0), (do, cut)))
    ]
    for c in shared:
        c.start()

    local = [
        pltpu.make_async_copy(wk, kwin.at[pl.ds(W, rows)], lsem.at[0]),
        pltpu.make_async_copy(wvT, vwin.at[:, pl.ds(W, rows)], lsem.at[1]),
    ]
    live = length[0]
    offset = sp * rows
    rowid = lax.broadcasted_iota(jnp.int32, (128, rows), 0) // DQK
    for h in range(heads):
        tile = dqT[(h // 2) * 128:(h // 2) * 128 + 128, :]
        for m in (0, 1):
            keep = jnp.where(rowid == (h % 2) * 2 + m, 1.0, 0.0).astype(BF16)
            qz[h, m] = tile * keep
    mx[...] = jnp.full(mx.shape, NEG, F32)
    acc[...] = jnp.zeros(acc.shape, F32)

    def block(ksrc, vsrc, origin):
        spo = ring_to_sp(origin, n)
        start = spo * rows
        kpos = start + lax.broadcasted_iota(jnp.int32, (rows, 1), 0)
        klive = kpos < live
        vpos = start + lax.broadcasted_iota(jnp.int32, (1, rows), 1)
        vlive = jnp.where(vpos < live, 1.0, 0.0).astype(BF16)
        ones = jnp.broadcast_to(vlive, (16, rows))

        def head(h, carry):
            kt = ksrc[:, pl.ds(pl.multiple_of((h // 2) * 128, 128), 128)]
            vt = vsrc[pl.ds(pl.multiple_of(h * HEAD, HEAD), HEAD), :] * vlive
            vx = jnp.concatenate([vt, ones], axis=0)
            for m in (0, 1):
                for q0 in range(0, rows, 256):
                    cols = pl.ds(q0, 256)
                    s = dot(kt, qz[h, m, :, cols])
                    s = jnp.where(klive, s, NEG)
                    old = mx[h, m, :, cols]
                    new = jnp.maximum(old, jnp.max(s, axis=0, keepdims=True))
                    p = jnp.exp2(s - new).astype(BF16)
                    acc[h, m, :, cols] = acc[h, m, :, cols] * jnp.exp2(old - new) + dot(vx, p)
                    mx[h, m, :, cols] = new
            return carry

        lax.fori_loop(0, heads, head, 0)

    block(dk, dvT, me)
    for c in local[:2]:
        c.start()
    for c in local[:2]:
        c.wait()
    for c in halos:
        c.wait()

    krel = lax.broadcasted_iota(jnp.int32, (3 * W, W), 0)
    qrel = lax.broadcasted_iota(jnp.int32, (3 * W, W), 1)
    band = jnp.abs(krel - W - qrel) <= W
    krow = lax.broadcasted_iota(jnp.int32, (1, 3 * W), 1)
    zeros = jnp.zeros((HEAD, GROUP * W), BF16)

    def qblock(b, carry):
        base = offset + b * W - W
        kp = base + krel
        allowed = band & (kp >= 0) & (kp < live)
        bias = jnp.where(allowed, 0.0, NEG)
        bias = jnp.concatenate([bias] * GROUP, axis=1)
        vp = base + krow
        vlive = jnp.where((vp >= 0) & (vp < live), 1.0, 0.0).astype(BF16)
        ones = jnp.broadcast_to(vlive, (16, 3 * W))
        qlane = offset + b * W + lax.broadcasted_iota(jnp.int32, (1, W), 1)
        qlive = qlane < live
        at = pl.multiple_of(b * W, W)
        for j in range(kvh):
            lo = j * HEAD // kw * kw
            ks = kwin[pl.ds(at, 3 * W), lo:lo + kw]
            vt = vwin[j * HEAD:(j + 1) * HEAD, pl.ds(at, 3 * W)] * vlive
            vx = jnp.concatenate([vt, ones], axis=0)
            q = jnp.concatenate(
                [wqT[(j * GROUP + g) * HEAD:(j * GROUP + g + 1) * HEAD, pl.ds(at, W)] for g in range(GROUP)],
                axis=1)
            if kw > HEAD:
                q = jnp.concatenate([q, zeros] if j % 2 == 0 else [zeros, q], axis=0)
            s = dot(ks, q) + bias
            snk = jnp.concatenate(
                [jnp.full((1, W), sink[j * GROUP + g] * LOG2E, F32) for g in range(GROUP)], axis=1)
            top = jnp.maximum(snk, jnp.max(s, axis=0, keepdims=True))
            p = jnp.exp2(s - top).astype(BF16)
            o = dot(vx, p)
            r = o[:HEAD] / (o[HEAD:HEAD + 1] + jnp.exp2(snk - top))
            for g in range(GROUP):
                piece = jnp.where(qlive, r[:, g * W:(g + 1) * W], 0.0).astype(BF16)
                out[(j * GROUP + g) * HEAD:(j * GROUP + g + 1) * HEAD, pl.ds(at, W)] = piece
        return carry

    lax.fori_loop(0, rows // W, qblock, 0)

    def step(s, carry):
        kcopy(0, s).wait_recv()
        kcopy(0, s + 1).start()
        vcopy(1, s).wait_recv()
        vcopy(1, s + 1).start()
        vcopy(0, s).wait_recv()
        kcopy(1, s).wait_recv()

        @pl.when(s < half - 2)
        def _():
            vcopy(0, s + 1).start()
            kcopy(1, s + 1).start()

        def side(i, c):
            origin = (me + n + (2 * i - 1) * (s + 1)) % n
            block(kbuf.at[origin], vbuf.at[origin], origin)
            return c

        lax.fori_loop(0, 2, side, 0)
        return carry

    lax.fori_loop(0, half - 1, step, 0)
    kcopy(0, half - 1).wait_recv()
    vcopy(1, half - 1).wait_recv()
    far = (me + half) % n
    block(kbuf.at[far], vbuf.at[far], far)

    qlive = offset + lax.broadcasted_iota(jnp.int32, (1, rows), 1) < live
    base = wqT.shape[0]
    for h in range(heads):
        a0 = acc[h, 0]
        a1 = acc[h, 1]
        t0 = a0[HEAD:HEAD + 1]
        t1 = a1[HEAD:HEAD + 1]
        mixed = a0[:HEAD] / t0 - lam[h] * (a1[:HEAD] / t1)
        ms = jnp.mean(mixed * mixed, axis=0, keepdims=True)
        r = mixed * lax.rsqrt(ms + EPS) * gain[...]
        out[base + h * HEAD:base + (h + 1) * HEAD, :] = jnp.where(qlive, r, 0.0).astype(BF16)

    hidden = out.shape[0]
    for c0 in range(0, hidden, 128):
        w = min(128, hidden - c0)
        out_rows[:, c0:c0 + w] = out[c0:c0 + w, :].T

    for d in (0, 1):
        for s in range(half):
            if s < half - 1 or d == 0:
                kcopy(d, s, s == 0).wait_send()
            if s < half - 1 or d == 1:
                vcopy(d, s, s == 0).wait_send()
    for c in shared:
        c.wait()


def attention(n, length, sink, lam, gain, wqT, wk, wvT, dqT, dk, dvT, wo, do):
    hidden = wqT.shape[0] + dqT.shape[0]
    rows = wk.shape[0]
    heads = dqT.shape[0] // HEAD
    half = n // 2
    return pl.pallas_call(
        functools.partial(attention_kernel, n),
        out_shape=(
            jax.ShapeDtypeStruct((rows, hidden), BF16),
            jax.ShapeDtypeStruct((hidden, wo.shape[1]), BF16),
        ),
        in_specs=[SM, SM, SM] + [VM] * 7 + [ANY] * 2,
        out_specs=(VM, ANY),
        scratch_shapes=[
            pltpu.VMEM((hidden, rows), BF16),
            pltpu.VMEM((n,) + dk.shape, BF16),
            pltpu.VMEM((n,) + dvT.shape, BF16),
            pltpu.VMEM((rows + 2 * WINDOW, wk.shape[1]), BF16),
            pltpu.VMEM((wvT.shape[0], rows + 2 * WINDOW), BF16),
            pltpu.VMEM((heads, 2, 128, rows), BF16),
            pltpu.VMEM((heads, 2, HEAD + 16, rows), F32),
            pltpu.VMEM((heads, 2, 1, rows), F32),
            pltpu.SemaphoreType.DMA((2, 2, half)),
            pltpu.SemaphoreType.DMA((2, 2, half)),
            pltpu.SemaphoreType.DMA((2, 4)),
            pltpu.SemaphoreType.DMA((2,)),
            pltpu.SemaphoreType.DMA((2, 2)),
        ],
        compiler_params=pltpu.CompilerParams(
            collective_id=1, has_side_effects=True, vmem_limit_bytes=60 * 1024 * 1024),
        name="attention",
    )(length, sink, lam, gain, wqT, wk, wvT, dqT, dk, dvT, wo, do)


def gather_kernel(
    xs, widths, x, *refs,
):
    weights = refs[:-13]
    wqT, wk, wvT, dqT, dk, dvT, seg, wbuf, acc, wsem, psem, xsem, rsem = refs[-13:]
    rows, feats = x.shape
    step_rows = 128
    steps = rows // step_rows
    tp = lax.axis_index("tp")
    core = tp % 2
    xi = tp // 2
    peer = xi * 2 + 1 - core
    others = [((xi + d) % xs) * 2 + core for d in range(1, xs)]
    barrier = pltpu.get_barrier_semaphore()
    for d in others + [peer]:
        pl.semaphore_signal(barrier, inc=1, device_id={"tp": d}, device_id_type=MESH)
    pl.semaphore_wait(barrier, xs)

    def across(c, d):
        part = pl.ds(pl.multiple_of(c * step_rows, step_rows), step_rows)
        return pltpu.make_async_remote_copy(
            src_ref=x.at[part], dst_ref=seg.at[tp, part], send_sem=xsem.at[0, d, c],
            recv_sem=xsem.at[1, d, c], device_id={"tp": others[d]}, device_id_type=MESH)

    def relay(c, d):
        source = ((xi + xs - d - 1) % xs) * 2 + core
        part = pl.ds(pl.multiple_of(c * step_rows, step_rows), step_rows)
        return pltpu.make_async_remote_copy(
            src_ref=seg.at[source, part], dst_ref=seg.at[source, part], send_sem=rsem.at[0, d, c],
            recv_sem=rsem.at[1, d, c], device_id={"tp": peer}, device_id_type=MESH)

    for c in range(steps):
        for d in range(xs - 1):
            across(c, d).start()
    beside = pltpu.make_async_remote_copy(
        src_ref=x, dst_ref=seg.at[tp], send_sem=psem.at[0], recv_sem=psem.at[1],
        device_id={"tp": peer}, device_id_type=MESH)
    beside.start()
    loads, at = [], 0
    for i, w in enumerate(weights):
        loads.append(pltpu.make_async_copy(w, wbuf.at[:, pl.ds(at, w.shape[1])], wsem.at[i]))
        at += w.shape[1]
    cuts = [(sum(widths[:i]), sum(widths[:i + 1])) for i in range(6)]
    for c in loads:
        c.start()
    for c in loads:
        c.wait()
    beside.wait_recv()

    def weight(t):
        return wbuf[pl.ds(pl.multiple_of(t * feats, feats), feats), :]

    def near(c, carry):
        part = pl.ds(pl.multiple_of(c * step_rows, step_rows), step_rows)
        acc[part, :] = dot(x[part, :], weight(tp)) + dot(seg[peer, part, :], weight(peer))
        return carry

    lax.fori_loop(0, steps, near, 0)

    def far(c, carry):
        part = pl.ds(pl.multiple_of(c * step_rows, step_rows), step_rows)
        total = acc[part, :]
        for d in range(xs - 1):
            source = (xi + xs - d - 1) % xs
            across(c, d).wait_recv()
            relay(c, d).start()
            total += dot(seg[source * 2 + core, part, :], weight(source * 2 + core))
            relay(c, d).wait_recv()
            total += dot(seg[source * 2 + 1 - core, part, :], weight(source * 2 + 1 - core))
        pieces = [total[:, a:b] for a, b in cuts]
        wqT[:, part] = (pieces[0] * (HEAD ** -0.5 * LOG2E)).T.astype(BF16)
        wk[part, :] = pieces[1].astype(BF16)
        wvT[:, part] = pieces[2].T.astype(BF16)
        dqT[:, part] = (pieces[3] * (DQK ** -0.5 * LOG2E)).T.astype(BF16)
        dk[part, :] = pieces[4].astype(BF16)
        dvT[:, part] = pieces[5].T.astype(BF16)
        return carry

    lax.fori_loop(0, steps, far, 0)
    beside.wait_send()
    for c in range(steps):
        for d in range(xs - 1):
            across(c, d).wait_send()
            relay(c, d).wait_send()


def gather(xs, x, *weights):
    rows, feats = x.shape
    widths = [w.shape[1] for w in weights]
    steps = rows // 128
    depth = weights[0].shape[0]
    if any(w % 128 for w in widths):
        weights = [jnp.concatenate(weights, axis=1)]
    shapes = [(widths[0], rows), (rows, widths[1]), (widths[2], rows),
              (widths[3], rows), (rows, widths[4]), (widths[5], rows)]
    return pl.pallas_call(
        functools.partial(gather_kernel, xs, widths),
        out_shape=[jax.ShapeDtypeStruct(s, BF16) for s in shapes],
        in_specs=[VM] + [ANY] * len(weights),
        out_specs=[VM] * 6,
        scratch_shapes=[
            pltpu.VMEM((2 * xs, rows, feats), BF16),
            pltpu.VMEM((depth, sum(widths)), BF16),
            pltpu.VMEM((rows, sum(widths)), F32),
            pltpu.SemaphoreType.DMA((6,)),
            pltpu.SemaphoreType.DMA((2,)),
            pltpu.SemaphoreType.DMA((2, xs - 1, steps)),
            pltpu.SemaphoreType.DMA((2, xs - 1, steps)),
        ],
        compiler_params=pltpu.CompilerParams(
            collective_id=2, has_side_effects=True, vmem_limit_bytes=60 * 1024 * 1024),
        name="gather",
    )(x, *weights)


def project_kernel(xs, parts, a, wo, do, wp, out, wbuf, ap, sbuf, rbuf, wsem, asem, ssem):
    rows, hidden = a.shape
    share = rows // (2 * xs)
    width = out.shape[1] // parts
    tp = lax.axis_index("tp")
    core = tp % 2
    xi = tp // 2
    peer = xi * 2 + 1 - core
    others = [((xi + d) % xs) * 2 + core for d in range(1, xs)]
    cut = wo.shape[0]

    def loads(j):
        cols = pl.ds(pl.multiple_of(j * width, width), width)
        return [
            pltpu.make_async_copy(src.at[:, cols], wbuf.at[pl.ds(at, src.shape[0]), cols], wsem.at[j, i])
            for i, (src, at) in enumerate(((wo, 0), (do, cut), (wp, hidden)))
        ]

    for j in range(parts):
        for c in loads(j):
            c.start()
    barrier = pltpu.get_barrier_semaphore()
    for d in others + [peer]:
        pl.semaphore_signal(barrier, inc=1, device_id={"tp": d}, device_id_type=MESH)
    pl.semaphore_wait(barrier, xs)

    def rows_of(block):
        return pl.ds(pl.multiple_of(block * share, share), share)

    swaps = [
        pltpu.make_async_remote_copy(
            src_ref=a.at[rows_of(c * 2 + 1 - core)], dst_ref=ap.at[c], send_sem=asem.at[0, c],
            recv_sem=asem.at[1, c], device_id={"tp": peer}, device_id_type=MESH)
        for c in range(xs)
    ]
    for c in swaps:
        c.start()
    for c in swaps:
        c.wait()

    def send(j, d):
        cols = pl.ds(pl.multiple_of(j * width, width), width)
        return pltpu.make_async_remote_copy(
            src_ref=sbuf.at[d, :, cols], dst_ref=rbuf.at[d, :, cols], send_sem=ssem.at[0, d, j],
            recv_sem=ssem.at[1, d, j], device_id={"tp": others[d]}, device_id_type=MESH)

    def product(chip, cols):
        lhs = jnp.concatenate([a[rows_of(chip * 2 + core), :], ap[chip]], axis=1)
        return dot(lhs, wbuf[:, cols])

    def remote(j, carry):
        for c in loads(j):
            c.wait()
        cols = pl.ds(pl.multiple_of(j * width, width), width)
        for d in range(xs - 1):
            sbuf[d, :, cols] = product((xi + d + 1) % xs, cols).astype(BF16)
            send(j, d).start()
        return carry

    lax.fori_loop(0, parts, remote, 0)

    def own(j, carry):
        cols = pl.ds(pl.multiple_of(j * width, width), width)
        total = product(xi, cols)
        for d in range(xs - 1):
            send(j, d).wait_recv()
            total += rbuf[d, :, cols].astype(F32)
        out[:, cols] = total.astype(BF16)
        return carry

    lax.fori_loop(0, parts, own, 0)
    for j in range(parts):
        for d in range(xs - 1):
            send(j, d).wait_send()


def project(xs, a, wo, do, wp):
    rows, hidden = a.shape
    share = rows // (2 * xs)
    model = wo.shape[1]
    parts = 8
    return pl.pallas_call(
        functools.partial(project_kernel, xs, parts),
        out_shape=jax.ShapeDtypeStruct((share, model), BF16),
        in_specs=[VM] + [ANY] * 3,
        out_specs=VM,
        scratch_shapes=[
            pltpu.VMEM((2 * hidden, model), BF16),
            pltpu.VMEM((xs, share, hidden), BF16),
            pltpu.VMEM((xs - 1, share, model), BF16),
            pltpu.VMEM((xs - 1, share, model), BF16),
            pltpu.SemaphoreType.DMA((parts, 3)),
            pltpu.SemaphoreType.DMA((2, xs)),
            pltpu.SemaphoreType.DMA((2, xs - 1, parts)),
        ],
        compiler_params=pltpu.CompilerParams(
            collective_id=3, has_side_effects=True, vmem_limit_bytes=60 * 1024 * 1024),
        name="project",
    )(a, wo, do, wp)


def body(n, xs, inputs, length, win_query, win_key, win_value, sink_logit, diff_query, diff_key,
         diff_value, mix_lambda, head_gain, win_out, diff_out):
    wqT, wk, wvT, dqT, dk, dvT = gather(
        xs, inputs, win_query, win_key, win_value, diff_query, diff_key, diff_value)
    rows, wp = attention(n, length, sink_logit, mix_lambda, head_gain.reshape(-1, 1),
                         wqT, wk, wvT, dqT, dk, dvT, win_out, diff_out)
    return project(xs, rows, win_out, diff_out, wp)


def solution(mesh):
    placed = (
        P("sp", "tp"), P(), P(None, "tp"), P(None, "tp"), P(None, "tp"), P("tp"), P(None, "tp"),
        P(None, "tp"), P(None, "tp"), P("tp"), P(), P("tp", None), P("tp", None),
    )
    return jax.shard_map(
        functools.partial(body, mesh.shape["sp"], mesh.shape["tp"] // 2), mesh=mesh, in_specs=placed,
        out_specs=P(("sp", "tp"), None), check_vma=False)
```

```python
import functools

import jax
import jax.numpy as jnp
from jax import lax
from jax.experimental import pallas as pl
from jax.experimental.pallas import tpu as pltpu
from jax.sharding import PartitionSpec as P

HEAD = 64
DQK = 32
GROUP = 3
WINDOW = 128
LOG2E = 1.4426950408889634
NEG = -1e30
EPS = 1e-06
MESH = pl.DeviceIdType.MESH
VM = pl.BlockSpec(memory_space=pltpu.VMEM)
ANY = pl.BlockSpec(memory_space=pl.ANY)
SM = pl.BlockSpec(memory_space=pltpu.SMEM)
F32 = jnp.float32
BF16 = jnp.bfloat16


def dot(a, b):
    return jnp.dot(a, b, preferred_element_type=F32)


def ring_to_sp(r, n):
    half = r // (n // 2)
    return (1 - half) * (2 * r) + half * (2 * (n - 1 - r) + 1)


def layer_kernel(n, xs, widths, length, sink, lam, gain, x, *refs):
    weights = refs[:-31]
    (wo, do, out_rows, wpeer, wqT, wk, wvT, dqT, dk, dvT, seg, wbuf, pacc, out, kbuf, vbuf, kwin, vwin, qz,
     acc, mx, ldsem, psem, xsem, rsem, csem, ksem, vsem, hsem, lsem, wsem) = refs[-31:]
    rows, feats = x.shape
    step_rows = 128
    steps = rows // step_rows
    heads = dqT.shape[0] // HEAD
    kvh = wk.shape[1] // HEAD
    kw = min(2 * HEAD, wk.shape[1])
    tp = lax.axis_index("tp")
    core = tp % 2
    xi = tp // 2
    peer = xi * 2 + 1 - core
    others = [((xi + d) % xs) * 2 + core for d in range(1, xs)]
    sp = lax.axis_index("sp")
    y = sp % 2
    z = sp // 2
    me = z + y * (n - 1 - 2 * z)
    half = n // 2
    right = ring_to_sp((me + 1) % n, n)
    left = ring_to_sp((me + n - 1) % n, n)
    nxt = (sp + 1) % n
    prv = (sp + n - 1) % n
    W = WINDOW
    barrier = pltpu.get_barrier_semaphore()
    for d in (left, right, prv, nxt):
        pl.semaphore_signal(barrier, inc=1, device_id={"sp": d}, device_id_type=MESH)
    for d in others + [peer]:
        pl.semaphore_signal(barrier, inc=1, device_id={"tp": d}, device_id_type=MESH)
    pl.semaphore_wait(barrier, 4 + xs)

    def first(kind, direction, c):
        part = pl.ds(pl.multiple_of(c * step_rows, step_rows), step_rows)
        src, dst = ((dk.at[part], kbuf.at[me, part]), (dvT.at[:, part], vbuf.at[me, :, part]))[kind]
        return pltpu.make_async_remote_copy(
            src_ref=src, dst_ref=dst, send_sem=csem.at[0, kind, direction, c],
            recv_sem=csem.at[1, kind, direction, c],
            device_id={"sp": (right, left)[direction]}, device_id_type=MESH)

    def hop(kind, direction, s):
        slot = (me + n - s) % n if direction == 0 else (me + s) % n
        buf, sem = ((kbuf, ksem), (vbuf, vsem))[kind]
        return pltpu.make_async_remote_copy(
            src_ref=buf.at[slot], dst_ref=buf.at[slot],
            send_sem=sem.at[0, direction, s], recv_sem=sem.at[1, direction, s],
            device_id={"sp": (right, left)[direction]}, device_id_type=MESH)

    def arrived(kind, direction, s):
        if isinstance(s, int):
            if s == 0:
                for c in range(steps):
                    first(kind, direction, c).wait_recv()
            else:
                hop(kind, direction, s).wait_recv()
            return

        @pl.when(s == 0)
        def _():
            for c in range(steps):
                first(kind, direction, c).wait_recv()

        @pl.when(s > 0)
        def _():
            hop(kind, direction, s).wait_recv()

    def across(c, d):
        part = pl.ds(pl.multiple_of(c * step_rows, step_rows), step_rows)
        return pltpu.make_async_remote_copy(
            src_ref=x.at[part], dst_ref=seg.at[tp, part], send_sem=xsem.at[0, d, c],
            recv_sem=xsem.at[1, d, c], device_id={"tp": others[d]}, device_id_type=MESH)

    def relay(c, d):
        source = ((xi + xs - d - 1) % xs) * 2 + core
        part = pl.ds(pl.multiple_of(c * step_rows, step_rows), step_rows)
        return pltpu.make_async_remote_copy(
            src_ref=seg.at[source, part], dst_ref=seg.at[source, part], send_sem=rsem.at[0, d, c],
            recv_sem=rsem.at[1, d, c], device_id={"tp": peer}, device_id_type=MESH)

    for c in range(steps):
        for d in range(xs - 1):
            across(c, d).start()
    beside = pltpu.make_async_remote_copy(
        src_ref=x, dst_ref=seg.at[tp], send_sem=psem.at[0], recv_sem=psem.at[1],
        device_id={"tp": peer}, device_id_type=MESH)
    beside.start()
    loads, at = [], 0
    for i, w in enumerate(weights):
        loads.append(pltpu.make_async_copy(w, wbuf.at[:, pl.ds(at, w.shape[1])], ldsem.at[i]))
        at += w.shape[1]
    cuts = [(sum(widths[:i]), sum(widths[:i + 1])) for i in range(6)]
    for c in loads:
        c.start()
    for c in loads:
        c.wait()
    beside.wait_recv()

    def weight(t):
        return wbuf[pl.ds(pl.multiple_of(t * feats, feats), feats), :]

    def near(c, carry):
        part = pl.ds(pl.multiple_of(c * step_rows, step_rows), step_rows)
        pacc[part, :] = dot(x[part, :], weight(tp)) + dot(seg[peer, part, :], weight(peer))
        return carry

    lax.fori_loop(0, steps, near, 0)

    def far(c, carry):
        part = pl.ds(pl.multiple_of(c * step_rows, step_rows), step_rows)
        total = pacc[part, :]
        for d in range(xs - 1):
            source = (xi + xs - d - 1) % xs
            across(c, d).wait_recv()
            relay(c, d).start()
            total += dot(seg[source * 2 + core, part, :], weight(source * 2 + core))
            relay(c, d).wait_recv()
            total += dot(seg[source * 2 + 1 - core, part, :], weight(source * 2 + 1 - core))
        pieces = [total[:, a:b] for a, b in cuts]
        dk[part, :] = pieces[4].astype(BF16)
        dvT[:, part] = pieces[5].T.astype(BF16)
        wqT[:, part] = (pieces[0] * (HEAD ** -0.5 * LOG2E)).T.astype(BF16)
        wk[part, :] = pieces[1].astype(BF16)
        wvT[:, part] = pieces[2].T.astype(BF16)
        dqT[:, part] = (pieces[3] * (DQK ** -0.5 * LOG2E)).T.astype(BF16)
        for d in (0, 1):
            first(0, d, c).start()
            first(1, d, c).start()
        return carry

    lax.fori_loop(0, steps, far, 0)

    halos = []
    for i, (src, dst, to) in enumerate((
        (wk.at[pl.ds(rows - W, W)], kwin.at[pl.ds(0, W)], nxt),
        (wvT.at[:, pl.ds(rows - W, W)], vwin.at[:, pl.ds(0, W)], nxt),
        (wk.at[pl.ds(0, W)], kwin.at[pl.ds(rows + W, W)], prv),
        (wvT.at[:, pl.ds(0, W)], vwin.at[:, pl.ds(rows + W, W)], prv),
    )):
        c = pltpu.make_async_remote_copy(
            src_ref=src, dst_ref=dst, send_sem=hsem.at[0, i], recv_sem=hsem.at[1, i],
            device_id={"sp": to}, device_id_type=MESH)
        c.start()
        halos.append(c)
    cut = wo.shape[0]
    shared = [
        pltpu.make_async_remote_copy(
            src_ref=src, dst_ref=wpeer.at[pl.ds(at, src.shape[0])], send_sem=wsem.at[0, i],
            recv_sem=wsem.at[1, i], device_id={"tp": peer}, device_id_type=MESH)
        for i, (src, at) in enumerate(((wo, 0), (do, cut)))
    ]
    for c in shared:
        c.start()
    local = [
        pltpu.make_async_copy(wk, kwin.at[pl.ds(W, rows)], lsem.at[0]),
        pltpu.make_async_copy(wvT, vwin.at[:, pl.ds(W, rows)], lsem.at[1]),
    ]
    for c in local:
        c.start()
    live = length[0]
    offset = sp * rows
    rowid = lax.broadcasted_iota(jnp.int32, (128, rows), 0) // DQK
    for h in range(heads):
        tile = dqT[(h // 2) * 128:(h // 2) * 128 + 128, :]
        for m in (0, 1):
            keep = jnp.where(rowid == (h % 2) * 2 + m, 1.0, 0.0).astype(BF16)
            qz[h, m] = tile * keep
    mx[...] = jnp.full(mx.shape, NEG, F32)
    acc[...] = jnp.zeros(acc.shape, F32)

    def block(ksrc, vsrc, origin):
        spo = ring_to_sp(origin, n)
        start = spo * rows
        kpos = start + lax.broadcasted_iota(jnp.int32, (rows, 1), 0)
        klive = kpos < live
        vpos = start + lax.broadcasted_iota(jnp.int32, (1, rows), 1)
        vlive = jnp.where(vpos < live, 1.0, 0.0).astype(BF16)
        ones = jnp.broadcast_to(vlive, (16, rows))

        def head(h, carry):
            kt = ksrc[:, pl.ds(pl.multiple_of((h // 2) * 128, 128), 128)]
            vt = vsrc[pl.ds(pl.multiple_of(h * HEAD, HEAD), HEAD), :] * vlive
            vx = jnp.concatenate([vt, ones], axis=0)
            for m in (0, 1):
                for q0 in range(0, rows, 256):
                    cols = pl.ds(q0, 256)
                    s = dot(kt, qz[h, m, :, cols])
                    s = jnp.where(klive, s, NEG)
                    old = mx[h, m, :, cols]
                    new = jnp.maximum(old, jnp.max(s, axis=0, keepdims=True))
                    p = jnp.exp2(s - new).astype(BF16)
                    acc[h, m, :, cols] = acc[h, m, :, cols] * jnp.exp2(old - new) + dot(vx, p)
                    mx[h, m, :, cols] = new
            return carry

        lax.fori_loop(0, heads, head, 0)

    block(dk, dvT, me)

    def relay_near(s):
        arrived(0, 0, s)
        hop(0, 0, s + 1).start()
        arrived(1, 1, s)
        hop(1, 1, s + 1).start()

    def relay_rest(s):
        arrived(1, 0, s)
        arrived(0, 1, s)

        @pl.when(s < half - 2)
        def _():
            hop(1, 0, s + 1).start()
            hop(0, 1, s + 1).start()

    relay_near(0)
    for c in local:
        c.wait()
    for c in halos:
        c.wait()

    krel = lax.broadcasted_iota(jnp.int32, (3 * W, W), 0)
    qrel = lax.broadcasted_iota(jnp.int32, (3 * W, W), 1)
    band = jnp.abs(krel - W - qrel) <= W
    krow = lax.broadcasted_iota(jnp.int32, (1, 3 * W), 1)
    zeros = jnp.zeros((HEAD, GROUP * W), BF16)

    def qblock(b, carry):
        base = offset + b * W - W
        kp = base + krel
        allowed = band & (kp >= 0) & (kp < live)
        bias = jnp.where(allowed, 0.0, NEG)
        bias = jnp.concatenate([bias] * GROUP, axis=1)
        vp = base + krow
        vlive = jnp.where((vp >= 0) & (vp < live), 1.0, 0.0).astype(BF16)
        ones = jnp.broadcast_to(vlive, (16, 3 * W))
        qlane = offset + b * W + lax.broadcasted_iota(jnp.int32, (1, W), 1)
        qlive = qlane < live
        at = pl.multiple_of(b * W, W)
        for j in range(kvh):
            lo = j * HEAD // kw * kw
            ks = kwin[pl.ds(at, 3 * W), lo:lo + kw]
            vt = vwin[j * HEAD:(j + 1) * HEAD, pl.ds(at, 3 * W)] * vlive
            vx = jnp.concatenate([vt, ones], axis=0)
            q = jnp.concatenate(
                [wqT[(j * GROUP + g) * HEAD:(j * GROUP + g + 1) * HEAD, pl.ds(at, W)] for g in range(GROUP)],
                axis=1)
            if kw > HEAD:
                q = jnp.concatenate([q, zeros] if j % 2 == 0 else [zeros, q], axis=0)
            s = dot(ks, q) + bias
            snk = jnp.concatenate(
                [jnp.full((1, W), sink[j * GROUP + g] * LOG2E, F32) for g in range(GROUP)], axis=1)
            top = jnp.maximum(snk, jnp.max(s, axis=0, keepdims=True))
            p = jnp.exp2(s - top).astype(BF16)
            o = dot(vx, p)
            r = o[:HEAD] / (o[HEAD:HEAD + 1] + jnp.exp2(snk - top))
            for g in range(GROUP):
                piece = jnp.where(qlive, r[:, g * W:(g + 1) * W], 0.0).astype(BF16)
                out[(j * GROUP + g) * HEAD:(j * GROUP + g + 1) * HEAD, pl.ds(at, W)] = piece
        return carry


    def step(s, carry):
        relay_rest(s)

        @pl.when(s == 0)
        def _():
            lax.fori_loop(0, rows // W, qblock, 0)

        def side(i, c):
            @pl.when((i == 1) & (s < half - 2))
            def _():
                hop(0, 0, s + 1).wait_recv()
                hop(0, 0, s + 2).start()
                hop(1, 1, s + 1).wait_recv()
                hop(1, 1, s + 2).start()

            origin = (me + n + (2 * i - 1) * (s + 1)) % n
            block(kbuf.at[origin], vbuf.at[origin], origin)
            return c

        lax.fori_loop(0, 2, side, 0)
        return carry

    lax.fori_loop(0, half - 1, step, 0)
    hop(0, 0, half - 1).wait_recv()
    hop(1, 1, half - 1).wait_recv()
    distant = (me + half) % n
    block(kbuf.at[distant], vbuf.at[distant], distant)

    qlive = offset + lax.broadcasted_iota(jnp.int32, (1, rows), 1) < live
    base = wqT.shape[0]
    for h in range(heads):
        a0 = acc[h, 0]
        a1 = acc[h, 1]
        t0 = a0[HEAD:HEAD + 1]
        t1 = a1[HEAD:HEAD + 1]
        mixed = a0[:HEAD] / t0 - lam[h] * (a1[:HEAD] / t1)
        ms = jnp.mean(mixed * mixed, axis=0, keepdims=True)
        r = mixed * lax.rsqrt(ms + EPS) * gain[...]
        out[base + h * HEAD:base + (h + 1) * HEAD, :] = jnp.where(qlive, r, 0.0).astype(BF16)

    hidden = out.shape[0]
    for c0 in range(0, hidden, 128):
        w = min(128, hidden - c0)
        out_rows[:, c0:c0 + w] = out[c0:c0 + w, :].T

    beside.wait_send()
    for c in range(steps):
        for d in range(xs - 1):
            across(c, d).wait_send()
            relay(c, d).wait_send()
        for d in (0, 1):
            first(0, d, c).wait_send()
            first(1, d, c).wait_send()
    for d in (0, 1):
        for s in range(1, half):
            if s < half - 1 or d == 0:
                hop(0, d, s).wait_send()
            if s < half - 1 or d == 1:
                hop(1, d, s).wait_send()
    for c in shared:
        c.wait()


def layer(n, xs, length, sink, lam, gain, x, weights, wo, do):
    rows, feats = x.shape
    widths = [w.shape[1] for w in weights]
    steps = rows // 128
    depth = weights[0].shape[0]
    if any(w % 128 for w in widths):
        weights = [jnp.concatenate(weights, axis=1)]
    hidden = wo.shape[0] + do.shape[0]
    heads = widths[3] // HEAD
    half = n // 2
    return pl.pallas_call(
        functools.partial(layer_kernel, n, xs, widths),
        out_shape=(
            jax.ShapeDtypeStruct((rows, hidden), BF16),
            jax.ShapeDtypeStruct((hidden, wo.shape[1]), BF16),
        ),
        in_specs=[SM, SM, SM, VM, VM] + [ANY] * (len(weights) + 2),
        out_specs=(VM, ANY),
        scratch_shapes=[
            pltpu.VMEM((widths[0], rows), BF16),
            pltpu.VMEM((rows, widths[1]), BF16),
            pltpu.VMEM((widths[2], rows), BF16),
            pltpu.VMEM((widths[3], rows), BF16),
            pltpu.VMEM((rows, widths[4]), BF16),
            pltpu.VMEM((widths[5], rows), BF16),
            pltpu.VMEM((2 * xs, rows, feats), BF16),
            pltpu.VMEM((depth, sum(widths)), BF16),
            pltpu.VMEM((rows, sum(widths)), F32),
            pltpu.VMEM((hidden, rows), BF16),
            pltpu.VMEM((n, rows, widths[4]), BF16),
            pltpu.VMEM((n, widths[5], rows), BF16),
            pltpu.VMEM((rows + 2 * WINDOW, widths[1]), BF16),
            pltpu.VMEM((widths[2], rows + 2 * WINDOW), BF16),
            pltpu.VMEM((heads, 2, 128, rows), BF16),
            pltpu.VMEM((heads, 2, HEAD + 16, rows), F32),
            pltpu.VMEM((heads, 2, 1, rows), F32),
            pltpu.SemaphoreType.DMA((6,)),
            pltpu.SemaphoreType.DMA((2,)),
            pltpu.SemaphoreType.DMA((2, xs - 1, steps)),
            pltpu.SemaphoreType.DMA((2, xs - 1, steps)),
            pltpu.SemaphoreType.DMA((2, 2, 2, steps)),
            pltpu.SemaphoreType.DMA((2, 2, half)),
            pltpu.SemaphoreType.DMA((2, 2, half)),
            pltpu.SemaphoreType.DMA((2, 4)),
            pltpu.SemaphoreType.DMA((2,)),
            pltpu.SemaphoreType.DMA((2, 2)),
        ],
        compiler_params=pltpu.CompilerParams(
            collective_id=1, has_side_effects=True, vmem_limit_bytes=60 * 1024 * 1024),
        name="layer",
    )(length, sink, lam, gain, x, *weights, wo, do)


def project_kernel(xs, parts, a, wo, do, wp, out, wbuf, ap, sbuf, rbuf, wsem, asem, ssem):
    rows, hidden = a.shape
    share = rows // (2 * xs)
    width = out.shape[1] // parts
    tp = lax.axis_index("tp")
    core = tp % 2
    xi = tp // 2
    peer = xi * 2 + 1 - core
    others = [((xi + d) % xs) * 2 + core for d in range(1, xs)]
    cut = wo.shape[0]

    def loads(j):
        cols = pl.ds(pl.multiple_of(j * width, width), width)
        return [
            pltpu.make_async_copy(src.at[:, cols], wbuf.at[pl.ds(at, src.shape[0]), cols], wsem.at[j, i])
            for i, (src, at) in enumerate(((wo, 0), (do, cut), (wp, hidden)))
        ]

    for j in range(parts):
        for c in loads(j):
            c.start()
    barrier = pltpu.get_barrier_semaphore()
    for d in others + [peer]:
        pl.semaphore_signal(barrier, inc=1, device_id={"tp": d}, device_id_type=MESH)
    pl.semaphore_wait(barrier, xs)

    def rows_of(block):
        return pl.ds(pl.multiple_of(block * share, share), share)

    swaps = [
        pltpu.make_async_remote_copy(
            src_ref=a.at[rows_of(c * 2 + 1 - core)], dst_ref=ap.at[c], send_sem=asem.at[0, c],
            recv_sem=asem.at[1, c], device_id={"tp": peer}, device_id_type=MESH)
        for c in range(xs)
    ]
    for c in swaps:
        c.start()
    for c in swaps:
        c.wait()

    def send(j, d):
        cols = pl.ds(pl.multiple_of(j * width, width), width)
        return pltpu.make_async_remote_copy(
            src_ref=sbuf.at[d, :, cols], dst_ref=rbuf.at[d, :, cols], send_sem=ssem.at[0, d, j],
            recv_sem=ssem.at[1, d, j], device_id={"tp": others[d]}, device_id_type=MESH)

    def product(chip, cols):
        lhs = jnp.concatenate([a[rows_of(chip * 2 + core), :], ap[chip]], axis=1)
        return dot(lhs, wbuf[:, cols])

    def remote(j, carry):
        for c in loads(j):
            c.wait()
        cols = pl.ds(pl.multiple_of(j * width, width), width)
        for d in range(xs - 1):
            sbuf[d, :, cols] = product((xi + d + 1) % xs, cols).astype(BF16)
            send(j, d).start()
        return carry

    lax.fori_loop(0, parts, remote, 0)

    def own(j, carry):
        cols = pl.ds(pl.multiple_of(j * width, width), width)
        total = product(xi, cols)
        for d in range(xs - 1):
            send(j, d).wait_recv()
            total += rbuf[d, :, cols].astype(F32)
        out[:, cols] = total.astype(BF16)
        return carry

    lax.fori_loop(0, parts, own, 0)
    for j in range(parts):
        for d in range(xs - 1):
            send(j, d).wait_send()


def project(xs, a, wo, do, wp):
    rows, hidden = a.shape
    share = rows // (2 * xs)
    model = wo.shape[1]
    parts = 8
    return pl.pallas_call(
        functools.partial(project_kernel, xs, parts),
        out_shape=jax.ShapeDtypeStruct((share, model), BF16),
        in_specs=[VM] + [ANY] * 3,
        out_specs=VM,
        scratch_shapes=[
            pltpu.VMEM((2 * hidden, model), BF16),
            pltpu.VMEM((xs, share, hidden), BF16),
            pltpu.VMEM((xs - 1, share, model), BF16),
            pltpu.VMEM((xs - 1, share, model), BF16),
            pltpu.SemaphoreType.DMA((parts, 3)),
            pltpu.SemaphoreType.DMA((2, xs)),
            pltpu.SemaphoreType.DMA((2, xs - 1, parts)),
        ],
        compiler_params=pltpu.CompilerParams(
            collective_id=3, has_side_effects=True, vmem_limit_bytes=60 * 1024 * 1024),
        name="project",
    )(a, wo, do, wp)


def body(n, xs, inputs, length, win_query, win_key, win_value, sink_logit, diff_query, diff_key,
         diff_value, mix_lambda, head_gain, win_out, diff_out):
    weights = [win_query, win_key, win_value, diff_query, diff_key, diff_value]
    rows, wp = layer(n, xs, length, sink_logit, mix_lambda, head_gain.reshape(-1, 1), inputs,
                     weights, win_out, diff_out)
    return project(xs, rows, win_out, diff_out, wp)


def solution(mesh):
    placed = (
        P("sp", "tp"), P(), P(None, "tp"), P(None, "tp"), P(None, "tp"), P("tp"), P(None, "tp"),
        P(None, "tp"), P(None, "tp"), P("tp"), P(), P("tp", None), P("tp", None),
    )
    return jax.shard_map(
        functools.partial(body, mesh.shape["sp"], mesh.shape["tp"] // 2), mesh=mesh, in_specs=placed,
        out_specs=P(("sp", "tp"), None), check_vma=False)
```

```python
import functools

import jax
import jax.numpy as jnp
from jax import lax
from jax.experimental import pallas as pl
from jax.experimental.pallas import tpu as pltpu
from jax.sharding import PartitionSpec as P

HEAD = 64
DQK = 32
GROUP = 3
WINDOW = 128
LOG2E = 1.4426950408889634
NEG = -1e30
EPS = 1e-06
MESH = pl.DeviceIdType.MESH
VM = pl.BlockSpec(memory_space=pltpu.VMEM)
ANY = pl.BlockSpec(memory_space=pl.ANY)
SM = pl.BlockSpec(memory_space=pltpu.SMEM)
F32 = jnp.float32
BF16 = jnp.bfloat16


def dot(a, b):
    return jnp.dot(a, b, preferred_element_type=F32)


def ring_to_sp(r, n):
    half = r // (n // 2)
    return (1 - half) * (2 * r) + half * (2 * (n - 1 - r) + 1)


def layer_kernel(n, xs, widths, length, sink, lam, gain, x, *refs):
    weights = refs[:-31]
    (wo, do, out_rows, wpeer, wqT, wk, wvT, dqT, dk, dvT, seg, wbuf, pacc, out, kbuf, vbuf, kwin, vwin, qz,
     acc, mx, ldsem, psem, xsem, rsem, csem, ksem, vsem, hsem, lsem, wsem) = refs[-31:]
    rows, feats = x.shape
    step_rows = 128
    steps = rows // step_rows
    heads = dqT.shape[0] // HEAD
    kvh = wk.shape[1] // HEAD
    kw = min(2 * HEAD, wk.shape[1])
    tp = lax.axis_index("tp")
    core = tp % 2
    xi = tp // 2
    peer = xi * 2 + 1 - core
    others = [((xi + d) % xs) * 2 + core for d in range(1, xs)]
    sp = lax.axis_index("sp")
    y = sp % 2
    z = sp // 2
    me = z + y * (n - 1 - 2 * z)
    half = n // 2
    right = ring_to_sp((me + 1) % n, n)
    left = ring_to_sp((me + n - 1) % n, n)
    nxt = (sp + 1) % n
    prv = (sp + n - 1) % n
    W = WINDOW
    barrier = pltpu.get_barrier_semaphore()
    for d in (left, right, prv, nxt):
        pl.semaphore_signal(barrier, inc=1, device_id={"sp": d}, device_id_type=MESH)
    for d in others + [peer]:
        pl.semaphore_signal(barrier, inc=1, device_id={"tp": d}, device_id_type=MESH)
    pl.semaphore_wait(barrier, 4 + xs)

    def first(kind, direction, c):
        part = pl.ds(pl.multiple_of(c * step_rows, step_rows), step_rows)
        src, dst = ((dk.at[part], kbuf.at[me, part]), (dvT.at[:, part], vbuf.at[me, :, part]))[kind]
        return pltpu.make_async_remote_copy(
            src_ref=src, dst_ref=dst, send_sem=csem.at[0, kind, direction, c],
            recv_sem=csem.at[1, kind, direction, c],
            device_id={"sp": (right, left)[direction]}, device_id_type=MESH)

    def hop(kind, direction, s):
        slot = (me + n - s) % n if direction == 0 else (me + s) % n
        buf, sem = ((kbuf, ksem), (vbuf, vsem))[kind]
        return pltpu.make_async_remote_copy(
            src_ref=buf.at[slot], dst_ref=buf.at[slot],
            send_sem=sem.at[0, direction, s], recv_sem=sem.at[1, direction, s],
            device_id={"sp": (right, left)[direction]}, device_id_type=MESH)

    def arrived(kind, direction, s):
        if isinstance(s, int):
            if s == 0:
                for c in range(steps):
                    first(kind, direction, c).wait_recv()
            else:
                hop(kind, direction, s).wait_recv()
            return

        @pl.when(s == 0)
        def _():
            for c in range(steps):
                first(kind, direction, c).wait_recv()

        @pl.when(s > 0)
        def _():
            hop(kind, direction, s).wait_recv()

    def across(c, d):
        part = pl.ds(pl.multiple_of(c * step_rows, step_rows), step_rows)
        return pltpu.make_async_remote_copy(
            src_ref=x.at[part], dst_ref=seg.at[tp, part], send_sem=xsem.at[0, d, c],
            recv_sem=xsem.at[1, d, c], device_id={"tp": others[d]}, device_id_type=MESH)

    def relay(c, d):
        source = ((xi + xs - d - 1) % xs) * 2 + core
        part = pl.ds(pl.multiple_of(c * step_rows, step_rows), step_rows)
        return pltpu.make_async_remote_copy(
            src_ref=seg.at[source, part], dst_ref=seg.at[source, part], send_sem=rsem.at[0, d, c],
            recv_sem=rsem.at[1, d, c], device_id={"tp": peer}, device_id_type=MESH)

    for c in range(steps):
        for d in range(xs - 1):
            across(c, d).start()
    beside = pltpu.make_async_remote_copy(
        src_ref=x, dst_ref=seg.at[tp], send_sem=psem.at[0], recv_sem=psem.at[1],
        device_id={"tp": peer}, device_id_type=MESH)
    beside.start()
    loads, at = [], 0
    for i, w in enumerate(weights):
        loads.append(pltpu.make_async_copy(w, wbuf.at[:, pl.ds(at, w.shape[1])], ldsem.at[i]))
        at += w.shape[1]
    cuts = [(sum(widths[:i]), sum(widths[:i + 1])) for i in range(6)]
    for c in loads:
        c.start()
    for c in loads:
        c.wait()
    beside.wait_recv()

    def weight(t):
        return wbuf[pl.ds(pl.multiple_of(t * feats, feats), feats), :]

    def near(c, carry):
        part = pl.ds(pl.multiple_of(c * step_rows, step_rows), step_rows)
        pacc[part, :] = dot(x[part, :], weight(tp)) + dot(seg[peer, part, :], weight(peer))
        return carry

    lax.fori_loop(0, steps, near, 0)

    def far(c, carry):
        part = pl.ds(pl.multiple_of(c * step_rows, step_rows), step_rows)
        total = pacc[part, :]
        for d in range(xs - 1):
            source = (xi + xs - d - 1) % xs
            across(c, d).wait_recv()
            relay(c, d).start()
            total += dot(seg[source * 2 + core, part, :], weight(source * 2 + core))
            relay(c, d).wait_recv()
            total += dot(seg[source * 2 + 1 - core, part, :], weight(source * 2 + 1 - core))
        pieces = [total[:, a:b] for a, b in cuts]
        dk[part, :] = pieces[4].astype(BF16)
        dvT[:, part] = pieces[5].T.astype(BF16)
        wqT[:, part] = (pieces[0] * (HEAD ** -0.5 * LOG2E)).T.astype(BF16)
        wk[part, :] = pieces[1].astype(BF16)
        wvT[:, part] = pieces[2].T.astype(BF16)
        dqT[:, part] = (pieces[3] * (DQK ** -0.5 * LOG2E)).T.astype(BF16)
        for d in (0, 1):
            first(0, d, c).start()
            first(1, d, c).start()
        return carry

    lax.fori_loop(0, steps, far, 0)

    halos = []
    for i, (src, dst, to) in enumerate((
        (wk.at[pl.ds(rows - W, W)], kwin.at[pl.ds(0, W)], nxt),
        (wvT.at[:, pl.ds(rows - W, W)], vwin.at[:, pl.ds(0, W)], nxt),
        (wk.at[pl.ds(0, W)], kwin.at[pl.ds(rows + W, W)], prv),
        (wvT.at[:, pl.ds(0, W)], vwin.at[:, pl.ds(rows + W, W)], prv),
    )):
        c = pltpu.make_async_remote_copy(
            src_ref=src, dst_ref=dst, send_sem=hsem.at[0, i], recv_sem=hsem.at[1, i],
            device_id={"sp": to}, device_id_type=MESH)
        c.start()
        halos.append(c)
    cut = wo.shape[0]
    shared = [
        pltpu.make_async_remote_copy(
            src_ref=src, dst_ref=wpeer.at[pl.ds(at, src.shape[0])], send_sem=wsem.at[0, i],
            recv_sem=wsem.at[1, i], device_id={"tp": peer}, device_id_type=MESH)
        for i, (src, at) in enumerate(((wo, 0), (do, cut)))
    ]
    for c in shared:
        c.start()
    local = [
        pltpu.make_async_copy(wk, kwin.at[pl.ds(W, rows)], lsem.at[0]),
        pltpu.make_async_copy(wvT, vwin.at[:, pl.ds(W, rows)], lsem.at[1]),
    ]
    for c in local:
        c.start()
    live = length[0]
    offset = sp * rows
    rowid = lax.broadcasted_iota(jnp.int32, (128, rows), 0) // DQK
    for h in range(heads):
        tile = dqT[(h // 2) * 128:(h // 2) * 128 + 128, :]
        for m in (0, 1):
            keep = jnp.where(rowid == (h % 2) * 2 + m, 1.0, 0.0).astype(BF16)
            qz[h, m] = tile * keep
    mx[...] = jnp.full(mx.shape, NEG, F32)
    acc[...] = jnp.zeros(acc.shape, F32)

    def block(ksrc, vsrc, origin):
        spo = ring_to_sp(origin, n)
        start = spo * rows
        kpos = start + lax.broadcasted_iota(jnp.int32, (rows, 1), 0)
        klive = kpos < live
        vpos = start + lax.broadcasted_iota(jnp.int32, (1, rows), 1)
        vlive = jnp.where(vpos < live, 1.0, 0.0).astype(BF16)
        ones = jnp.broadcast_to(vlive, (16, rows))

        def head(h, carry):
            kt = ksrc[:, pl.ds(pl.multiple_of((h // 2) * 128, 128), 128)]
            vt = vsrc[pl.ds(pl.multiple_of(h * HEAD, HEAD), HEAD), :] * vlive
            vx = jnp.concatenate([vt, ones], axis=0)
            tiles = [(m, q0) for m in (0, 1) for q0 in range(0, rows, 512)]
            nexts = dot(kt, qz[h, 0, :, pl.ds(0, 512)])
            for i, (m, q0) in enumerate(tiles):
                s = nexts
                if i + 1 < len(tiles):
                    m1, q1 = tiles[i + 1]
                    nexts = dot(kt, qz[h, m1, :, pl.ds(q1, 512)])
                cols = pl.ds(q0, 512)
                s = jnp.where(klive, s, NEG)
                old = mx[h, m, :, cols]
                new = jnp.maximum(old, jnp.max(s, axis=0, keepdims=True))
                p = jnp.exp2(s - new).astype(BF16)
                acc[h, m, :, cols] = acc[h, m, :, cols] * jnp.exp2(old - new) + dot(vx, p)
                mx[h, m, :, cols] = new
            return carry

        lax.fori_loop(0, heads, head, 0)

    block(dk, dvT, me)

    def relay_near(s):
        arrived(0, 0, s)
        hop(0, 0, s + 1).start()
        arrived(1, 1, s)
        hop(1, 1, s + 1).start()

    def relay_rest(s):
        arrived(1, 0, s)
        arrived(0, 1, s)

        @pl.when(s < half - 2)
        def _():
            hop(1, 0, s + 1).start()
            hop(0, 1, s + 1).start()

    relay_near(0)
    for c in local:
        c.wait()
    for c in halos:
        c.wait()

    krel = lax.broadcasted_iota(jnp.int32, (3 * W, W), 0)
    qrel = lax.broadcasted_iota(jnp.int32, (3 * W, W), 1)
    band = jnp.abs(krel - W - qrel) <= W
    krow = lax.broadcasted_iota(jnp.int32, (1, 3 * W), 1)
    zeros = jnp.zeros((HEAD, GROUP * W), BF16)

    def qblock(b, carry):
        base = offset + b * W - W
        kp = base + krel
        allowed = band & (kp >= 0) & (kp < live)
        bias = jnp.where(allowed, 0.0, NEG)
        bias = jnp.concatenate([bias] * GROUP, axis=1)
        vp = base + krow
        vlive = jnp.where((vp >= 0) & (vp < live), 1.0, 0.0).astype(BF16)
        ones = jnp.broadcast_to(vlive, (16, 3 * W))
        qlane = offset + b * W + lax.broadcasted_iota(jnp.int32, (1, W), 1)
        qlive = qlane < live
        at = pl.multiple_of(b * W, W)
        for j in range(kvh):
            lo = j * HEAD // kw * kw
            ks = kwin[pl.ds(at, 3 * W), lo:lo + kw]
            vt = vwin[j * HEAD:(j + 1) * HEAD, pl.ds(at, 3 * W)] * vlive
            vx = jnp.concatenate([vt, ones], axis=0)
            q = jnp.concatenate(
                [wqT[(j * GROUP + g) * HEAD:(j * GROUP + g + 1) * HEAD, pl.ds(at, W)] for g in range(GROUP)],
                axis=1)
            if kw > HEAD:
                q = jnp.concatenate([q, zeros] if j % 2 == 0 else [zeros, q], axis=0)
            s = dot(ks, q) + bias
            snk = jnp.concatenate(
                [jnp.full((1, W), sink[j * GROUP + g] * LOG2E, F32) for g in range(GROUP)], axis=1)
            top = jnp.maximum(snk, jnp.max(s, axis=0, keepdims=True))
            p = jnp.exp2(s - top).astype(BF16)
            o = dot(vx, p)
            r = o[:HEAD] / (o[HEAD:HEAD + 1] + jnp.exp2(snk - top))
            for g in range(GROUP):
                piece = jnp.where(qlive, r[:, g * W:(g + 1) * W], 0.0).astype(BF16)
                out[(j * GROUP + g) * HEAD:(j * GROUP + g + 1) * HEAD, pl.ds(at, W)] = piece
        return carry


    def step(s, carry):
        relay_rest(s)

        @pl.when(s == 0)
        def _():
            lax.fori_loop(0, rows // W, qblock, 0)

        def side(i, c):
            @pl.when((i == 1) & (s < half - 2))
            def _():
                hop(0, 0, s + 1).wait_recv()
                hop(0, 0, s + 2).start()
                hop(1, 1, s + 1).wait_recv()
                hop(1, 1, s + 2).start()

            origin = (me + n + (2 * i - 1) * (s + 1)) % n
            block(kbuf.at[origin], vbuf.at[origin], origin)
            return c

        lax.fori_loop(0, 2, side, 0)
        return carry

    lax.fori_loop(0, half - 1, step, 0)
    hop(0, 0, half - 1).wait_recv()
    hop(1, 1, half - 1).wait_recv()
    distant = (me + half) % n
    block(kbuf.at[distant], vbuf.at[distant], distant)

    qlive = offset + lax.broadcasted_iota(jnp.int32, (1, rows), 1) < live
    base = wqT.shape[0]
    column = jnp.broadcast_to(gain[...], (128, HEAD)).T[:, 0:1]
    for h in range(heads):
        a0 = acc[h, 0]
        a1 = acc[h, 1]
        t0 = a0[HEAD:HEAD + 1]
        t1 = a1[HEAD:HEAD + 1]
        mixed = a0[:HEAD] / t0 - lam[h] * (a1[:HEAD] / t1)
        ms = jnp.mean(mixed * mixed, axis=0, keepdims=True)
        r = mixed * lax.rsqrt(ms + EPS) * column
        out[base + h * HEAD:base + (h + 1) * HEAD, :] = jnp.where(qlive, r, 0.0).astype(BF16)

    hidden = out.shape[0]
    for c0 in range(0, hidden, 128):
        w = min(128, hidden - c0)
        out_rows[:, c0:c0 + w] = out[c0:c0 + w, :].T

    beside.wait_send()
    for c in range(steps):
        for d in range(xs - 1):
            across(c, d).wait_send()
            relay(c, d).wait_send()
        for d in (0, 1):
            first(0, d, c).wait_send()
            first(1, d, c).wait_send()
    for d in (0, 1):
        for s in range(1, half):
            if s < half - 1 or d == 0:
                hop(0, d, s).wait_send()
            if s < half - 1 or d == 1:
                hop(1, d, s).wait_send()
    for c in shared:
        c.wait()


def layer(n, xs, length, sink, lam, gain, x, weights, wo, do):
    rows, feats = x.shape
    widths = [w.shape[1] for w in weights]
    steps = rows // 128
    depth = weights[0].shape[0]
    if any(w % 128 for w in widths):
        weights = [jnp.concatenate(weights, axis=1)]
    hidden = wo.shape[0] + do.shape[0]
    heads = widths[3] // HEAD
    half = n // 2
    return pl.pallas_call(
        functools.partial(layer_kernel, n, xs, widths),
        out_shape=(
            jax.ShapeDtypeStruct((rows, hidden), BF16),
            jax.ShapeDtypeStruct((hidden, wo.shape[1]), BF16),
        ),
        in_specs=[SM, SM, SM, VM, VM] + [ANY] * (len(weights) + 2),
        out_specs=(VM, ANY),
        scratch_shapes=[
            pltpu.VMEM((widths[0], rows), BF16),
            pltpu.VMEM((rows, widths[1]), BF16),
            pltpu.VMEM((widths[2], rows), BF16),
            pltpu.VMEM((widths[3], rows), BF16),
            pltpu.VMEM((rows, widths[4]), BF16),
            pltpu.VMEM((widths[5], rows), BF16),
            pltpu.VMEM((2 * xs, rows, feats), BF16),
            pltpu.VMEM((depth, sum(widths)), BF16),
            pltpu.VMEM((rows, sum(widths)), F32),
            pltpu.VMEM((hidden, rows), BF16),
            pltpu.VMEM((n, rows, widths[4]), BF16),
            pltpu.VMEM((n, widths[5], rows), BF16),
            pltpu.VMEM((rows + 2 * WINDOW, widths[1]), BF16),
            pltpu.VMEM((widths[2], rows + 2 * WINDOW), BF16),
            pltpu.VMEM((heads, 2, 128, rows), BF16),
            pltpu.VMEM((heads, 2, HEAD + 16, rows), F32),
            pltpu.VMEM((heads, 2, 1, rows), F32),
            pltpu.SemaphoreType.DMA((6,)),
            pltpu.SemaphoreType.DMA((2,)),
            pltpu.SemaphoreType.DMA((2, xs - 1, steps)),
            pltpu.SemaphoreType.DMA((2, xs - 1, steps)),
            pltpu.SemaphoreType.DMA((2, 2, 2, steps)),
            pltpu.SemaphoreType.DMA((2, 2, half)),
            pltpu.SemaphoreType.DMA((2, 2, half)),
            pltpu.SemaphoreType.DMA((2, 4)),
            pltpu.SemaphoreType.DMA((2,)),
            pltpu.SemaphoreType.DMA((2, 2)),
        ],
        compiler_params=pltpu.CompilerParams(
            collective_id=1, has_side_effects=True, vmem_limit_bytes=60 * 1024 * 1024),
        name="layer",
    )(length, sink, lam, gain, x, *weights, wo, do)


def project_kernel(xs, parts, a, wo, do, wp, out, wbuf, ap, sbuf, rbuf, wsem, asem, ssem):
    rows, hidden = a.shape
    share = rows // (2 * xs)
    width = out.shape[1] // parts
    tp = lax.axis_index("tp")
    core = tp % 2
    xi = tp // 2
    peer = xi * 2 + 1 - core
    others = [((xi + d) % xs) * 2 + core for d in range(1, xs)]
    cut = wo.shape[0]

    def loads(j):
        cols = pl.ds(pl.multiple_of(j * width, width), width)
        return [
            pltpu.make_async_copy(src.at[:, cols], wbuf.at[pl.ds(at, src.shape[0]), cols], wsem.at[j, i])
            for i, (src, at) in enumerate(((wo, 0), (do, cut), (wp, hidden)))
        ]

    for j in range(parts):
        for c in loads(j):
            c.start()
    barrier = pltpu.get_barrier_semaphore()
    for d in others + [peer]:
        pl.semaphore_signal(barrier, inc=1, device_id={"tp": d}, device_id_type=MESH)
    pl.semaphore_wait(barrier, xs)

    def rows_of(block):
        return pl.ds(pl.multiple_of(block * share, share), share)

    swaps = [
        pltpu.make_async_remote_copy(
            src_ref=a.at[rows_of(c * 2 + 1 - core)], dst_ref=ap.at[c], send_sem=asem.at[0, c],
            recv_sem=asem.at[1, c], device_id={"tp": peer}, device_id_type=MESH)
        for c in range(xs)
    ]
    for c in swaps:
        c.start()
    for c in swaps:
        c.wait()

    def send(j, d):
        cols = pl.ds(pl.multiple_of(j * width, width), width)
        return pltpu.make_async_remote_copy(
            src_ref=sbuf.at[d, :, cols], dst_ref=rbuf.at[d, :, cols], send_sem=ssem.at[0, d, j],
            recv_sem=ssem.at[1, d, j], device_id={"tp": others[d]}, device_id_type=MESH)

    def product(chip, cols):
        lhs = jnp.concatenate([a[rows_of(chip * 2 + core), :], ap[chip]], axis=1)
        return dot(lhs, wbuf[:, cols])

    def remote(j, carry):
        for c in loads(j):
            c.wait()
        cols = pl.ds(pl.multiple_of(j * width, width), width)
        for d in range(xs - 1):
            sbuf[d, :, cols] = product((xi + d + 1) % xs, cols).astype(BF16)
            send(j, d).start()
        return carry

    lax.fori_loop(0, parts, remote, 0)

    def own(j, carry):
        cols = pl.ds(pl.multiple_of(j * width, width), width)
        total = product(xi, cols)
        for d in range(xs - 1):
            send(j, d).wait_recv()
            total += rbuf[d, :, cols].astype(F32)
        out[:, cols] = total.astype(BF16)
        return carry

    lax.fori_loop(0, parts, own, 0)
    for j in range(parts):
        for d in range(xs - 1):
            send(j, d).wait_send()


def project(xs, a, wo, do, wp):
    rows, hidden = a.shape
    share = rows // (2 * xs)
    model = wo.shape[1]
    parts = 8
    return pl.pallas_call(
        functools.partial(project_kernel, xs, parts),
        out_shape=jax.ShapeDtypeStruct((share, model), BF16),
        in_specs=[VM] + [ANY] * 3,
        out_specs=VM,
        scratch_shapes=[
            pltpu.VMEM((2 * hidden, model), BF16),
            pltpu.VMEM((xs, share, hidden), BF16),
            pltpu.VMEM((xs - 1, share, model), BF16),
            pltpu.VMEM((xs - 1, share, model), BF16),
            pltpu.SemaphoreType.DMA((parts, 3)),
            pltpu.SemaphoreType.DMA((2, xs)),
            pltpu.SemaphoreType.DMA((2, xs - 1, parts)),
        ],
        compiler_params=pltpu.CompilerParams(
            collective_id=3, has_side_effects=True, vmem_limit_bytes=60 * 1024 * 1024),
        name="project",
    )(a, wo, do, wp)


def body(n, xs, inputs, length, win_query, win_key, win_value, sink_logit, diff_query, diff_key,
         diff_value, mix_lambda, head_gain, win_out, diff_out):
    weights = [win_query, win_key, win_value, diff_query, diff_key, diff_value]
    rows, wp = layer(n, xs, length, sink_logit, mix_lambda, head_gain.reshape(1, -1), inputs,
                     weights, win_out, diff_out)
    return project(xs, rows, win_out, diff_out, wp)


def solution(mesh):
    placed = (
        P("sp", "tp"), P(), P(None, "tp"), P(None, "tp"), P(None, "tp"), P("tp"), P(None, "tp"),
        P(None, "tp"), P(None, "tp"), P("tp"), P(), P("tp", None), P("tp", None),
    )
    return jax.shard_map(
        functools.partial(body, mesh.shape["sp"], mesh.shape["tp"] // 2), mesh=mesh, in_specs=placed,
        out_specs=P(("sp", "tp"), None), check_vma=False)
```
